128 devices in a mesh: ep: 128 (over z, y, x, core).
Axes of the slice: x: 4, y: 4, z: 4, core: 2. Of those that a mesh axis runs over, the one named last changes fastest.
Arguments:
- tokens: bfloat16 [512, 2048], P('ep'), may hold values from -6 to 6
- lengths: int32 [512], P('ep'), may hold values from 1 to 1023
- cache_keys: bfloat16 [512, 1024, 2, 128], P('ep')
- cache_values: bfloat16 [512, 1024, 2, 128], P('ep'), may hold values from -6 to 6
- query_w: bfloat16 [2048, 1024], replicated, may hold values from -0.125 to 0.125
- key_w: bfloat16 [2048, 256], replicated, may hold values from -0.125 to 0.125
- value_w: bfloat16 [2048, 256], replicated, may hold values from -0.125 to 0.125
- out_w: bfloat16 [1024, 2048], replicated, may hold values from -0.1875 to 0.1875
- mix_lambda: float32 [8], replicated, may hold values from 0.3 to 0.8
- head_gain: float32 [128], replicated, may hold values from 0.1 to 1.9
- attn_gain: float32 [2048], replicated, may hold values from 0.1 to 1.9
- ffn_gain: float32 [2048], replicated, may hold values from 0.1 to 1.9
- routes: int32 [512, 2], P('ep'), may hold values from 0 to 7, all different within a row; in each aligned block of 4 rows (0 to 3, 4 to 7, ...) at most 2 rows name the same one
- route_weights: float32 [512, 2], P('ep'), may hold values from 0.2 to 1
- exp_gate: bfloat16 [2048, 49152], P(None, 'ep'), may hold values from -0.125 to 0.125
- exp_up: bfloat16 [2048, 49152], P(None, 'ep'), may hold values from -0.125 to 0.125
- exp_down: bfloat16 [49152, 2048], P('ep'), may hold values from -0.078125 to 0.078125
- dense_gate: bfloat16 [128, 256, 352], P('ep'), may hold values from -0.125 to 0.125
- dense_up: bfloat16 [128, 256, 352], P('ep'), may hold values from -0.125 to 0.125
- dense_down: bfloat16 [128, 352, 256], P('ep'), may hold values from -0.078125 to 0.078125
- branch_gate: bfloat16 [2048], replicated, may hold values from -0.125 to 0.125
Outputs:
- output: bfloat16 [512, 2048], P('ep')
- new_keys: bfloat16 [512, 256], P('ep')
- new_values: bfloat16 [512, 256], P('ep')
The draws below stay inside these ranges and needn't reach their ends.
Inputs may be any that keep to these rules, and one draw needn't show every extreme that they name: `routes`: each row names 2 different experts; among the 4 rows of one device no expert is named by more than 2 rows, a bound that some block reaches.
All inputs are finite; a program needn't handle non-finite values.
Results may differ from the reference program's by a relative error of at most 0.015.
Values may be sent and summed in bfloat16 or wider, within the bound.
A program may use at most 128 MiB of HBM per device.

```python
import math
import jax
import jax.numpy as jnp
import numpy as np
from jax import lax

D = 2048
HEADS = 8
KV_HEADS = 2
HEAD_DIM = 128
CACHE = 1024
SEQ_DEV = 4
TOP_K = 2
SPLIT = 16
EXP_FF = 6144
DENSE_FF = 5632
EXPERTS = 8
BLOCKS = 8
CAP = 2
TOKENS = 512
N_EP = 128


def draw_cache_keys(key, part):
    shape = (TOKENS, CACHE, KV_HEADS, HEAD_DIM)
    base_key = jax.random.fold_in(jax.random.fold_in(key, 11), 0)
    values = jax.random.normal(base_key, shape, jnp.float32) * 1.75
    values = jnp.clip(values, -10.0, 10.0)
    return values.astype(jnp.bfloat16)


def plant(drawn, stream_key, least, high):
    longest = drawn.shape.index(max(drawn.shape))
    spots = []
    for shift in (0, 1):
        where = [jax.random.randint(jax.random.fold_in(stream_key, axis), (), 0, length) for axis, length in enumerate(drawn.shape)]
        where[longest] = (where[longest] + shift) % drawn.shape[longest]
        spots.append(tuple(where))
    return drawn.at[spots[0]].set(least).at[spots[1]].set(high)


def level_of(key, extent, cuts, low, top_value):
    level = 1.0
    for position, blocks in cuts:
        steps = jax.random.uniform(jax.random.fold_in(jax.random.fold_in(key, 6), position), (blocks,), jnp.float32, low / len(cuts), top_value / len(cuts))
        level = level * jnp.repeat(jnp.exp(steps), extent[position] // blocks).reshape((-1,) + (1,) * (len(extent) - 1 - position))
    return level


def deal_out(own_key, own, number, rows, number_of, top, most, lean):
    ranking = jax.random.permutation(own_key, number_of)
    packed, ordinary = load_shares(number_of, rows * top, most, lean, True), load_shares(number_of, rows * top, most, lean, False)
    places = jnp.arange(number_of)

    def named(sizes, offset_by):
        used = int((sizes > 0).sum())
        fixed = max(1, used // 4)
        passed = fixed + (places - fixed + offset_by * (used - fixed)) % max(1, number_of - fixed)
        return jnp.zeros((number_of,), jnp.int32).at[ranking[jnp.where(places < fixed, places, passed)]].set(jnp.asarray(sizes, jnp.int32))

    sizes = jnp.where(number % 4 == 0, named(packed, number // 4), named(ordinary, number - number // 4 - 1))
    mixed = jax.random.permutation(jax.random.fold_in(own, 3), number_of)
    source_of, receiver = mixed[0:number_of // 2 * 2:2], mixed[1:number_of // 2 * 2:2]
    slack = jnp.minimum(sizes[source_of] - 1, most - sizes[receiver]) // 2
    slack = jnp.where((source_of == ranking[0]) | (receiver == ranking[0]) | (sizes[receiver] == 0), 0, jnp.maximum(slack, 0))
    passed = jax.random.randint(jax.random.fold_in(own, 4), (number_of // 2,), 0, 1 << 20) % (slack + 1)
    sizes = sizes.at[source_of].add(-passed).at[receiver].add(passed)
    members = jnp.searchsorted(jnp.cumsum(sizes), jnp.arange(rows * top), side="right").astype(jnp.int32)
    listing = members.reshape(top, rows).T
    listing = listing[jax.random.permutation(jax.random.fold_in(own, 1), rows)]
    offset_by = jax.random.randint(jax.random.fold_in(own, 2), (rows, 1), 0, top)
    return jnp.take_along_axis(listing, (jnp.arange(top)[None, :] + offset_by) % top, axis=1)


def load_shares(count, total, limit, skew, full):
    loads = [(1 << 20) // math.isqrt(grade ** skew) + 1 for grade in range(1, count + 1)]
    largest = limit if full else min(limit, max(-(-total // count), total * loads[0] // sum(loads)))
    least = 1 if total - largest >= count - 1 else 0
    counts, spare = [largest] + [least] * (count - 1), total - largest - least * (count - 1)
    while spare > 0:
        free = [i for i in range(1, count) if counts[i] < largest] or [i for i in range(1, count) if counts[i] < limit]
        mass, left = sum([loads[i] for i in free]), spare
        for i in free:
            extra = min(limit - counts[i], max(1, left * loads[i] // mass), spare)
            counts[i] = counts[i] + extra
            spare = spare - extra
    return np.array(counts)


def centred(key, extent, spread, most, shards=(), kind=jnp.bfloat16):
    values = jax.random.normal(key, extent, jnp.float32) * spread
    if len(shards) > 0:
        values = level_of(key, extent, shards, -0.22, 0.18) * values
    return jnp.clip(values, min=-most, max=most).astype(kind)


def setup_inputs(seed: int = 0) -> dict:
    seeds = jax.random.split(jax.random.key(seed), 22)
    tokens = centred(seeds[0], (TOKENS, D), 1.0, 6.0, ((0, 128),))
    lengths = plant(jax.random.randint(seeds[1], (TOKENS,), 1, CACHE), jax.random.fold_in(seeds[1], 1), 1, CACHE - 1).astype(jnp.int32)
    cache_keys = draw_cache_keys(jax.random.fold_in(seeds[21], 71), 0)
    cache_values = centred(seeds[3], (TOKENS, CACHE, KV_HEADS, HEAD_DIM), 1.0, 6.0, ((0, 128),))
    query_w = centred(seeds[4], (D, HEADS * HEAD_DIM), D ** -0.5, 0.125)
    key_w = centred(seeds[5], (D, KV_HEADS * HEAD_DIM), D ** -0.5, 0.125)
    value_w = centred(seeds[6], (D, KV_HEADS * HEAD_DIM), D ** -0.5, 0.125)
    out_w = centred(seeds[7], (HEADS * HEAD_DIM, D), (HEADS * HEAD_DIM) ** -0.5, 0.1875)
    mix_lambda = jnp.clip(jax.random.uniform(seeds[8], (HEADS,), jnp.float32, 0.3, 0.8), 0.3, 0.8)
    head_gain = jnp.clip(1.0 + 0.18 * jax.random.normal(seeds[9], (HEAD_DIM,), jnp.float32), 0.1, 1.9)
    attn_gain = jnp.clip(1.0 + 0.18 * jax.random.normal(seeds[10], (D,), jnp.float32), 0.1, 1.9)
    ffn_gain = jnp.clip(1.0 + 0.18 * jax.random.normal(seeds[11], (D,), jnp.float32), 0.1, 1.9)
    routes_keys = jax.random.split(jax.random.fold_in(seeds[12], 1), TOKENS // SEQ_DEV)
    routes_turns = jax.random.permutation(jax.random.fold_in(seeds[12], 3), TOKENS // SEQ_DEV)
    routes = jax.vmap(lambda own, number: deal_out(jax.random.fold_in(seeds[12], 2), own, number, SEQ_DEV, EXPERTS, TOP_K, CAP, 1))(routes_keys, routes_turns).reshape((TOKENS, TOP_K))
    route_weights = jnp.clip(0.2 + 0.8 * jax.random.uniform(seeds[13], (TOKENS, TOP_K), jnp.float32) ** level_of(seeds[13], (TOKENS, TOP_K), ((0, 128),), -0.2, 0.2), 0.2, 1.0)
    exp_gate = centred(seeds[14], (D, EXPERTS * EXP_FF), D ** -0.5, 0.125, ((1, 128),))
    exp_up = centred(seeds[15], (D, EXPERTS * EXP_FF), D ** -0.5, 0.125, ((1, 128),))
    exp_down = centred(seeds[16], (EXPERTS * EXP_FF, D), EXP_FF ** -0.5, 0.078125, ((0, 128),))
    dense_gate = centred(seeds[17], (N_EP, D // BLOCKS, DENSE_FF // SPLIT), D ** -0.5, 0.125, ((0, 128),))
    dense_up = centred(seeds[18], (N_EP, D // BLOCKS, DENSE_FF // SPLIT), D ** -0.5, 0.125, ((0, 128),))
    dense_down = centred(seeds[19], (N_EP, DENSE_FF // SPLIT, D // BLOCKS), DENSE_FF ** -0.5, 0.078125, ((0, 128),))
    branch_gate = centred(seeds[20], (D,), D ** -0.5, 0.125)
    return {"tokens": tokens, "lengths": lengths, "cache_keys": cache_keys, "cache_values": cache_values, "query_w": query_w, "key_w": key_w, "value_w": value_w, "out_w": out_w, "mix_lambda": mix_lambda, "head_gain": head_gain, "attn_gain": attn_gain, "ffn_gain": ffn_gain, "routes": routes, "route_weights": route_weights, "exp_gate": exp_gate, "exp_up": exp_up, "exp_down": exp_down, "dense_gate": dense_gate, "dense_up": dense_up, "dense_down": dense_down, "branch_gate": branch_gate}


def rms_norm(values, gain, epsilon):
    scale = lax.rsqrt(lax.optimization_barrier(jnp.mean(values * values, axis=-1, keepdims=True)) + epsilon)
    return values * scale * gain.astype(jnp.float32)

def softmax_pair(scores, own_score, valid):
    masked = jnp.where(valid, scores, -jnp.inf)
    largest = jnp.maximum(lax.optimization_barrier(jnp.max(masked, axis=-1)), own_score)
    raised = jnp.where(valid, jnp.exp(scores - largest[..., None]), 0.0)
    own_raised = jnp.exp(own_score - largest)
    total = lax.optimization_barrier(jnp.sum(raised, axis=-1)) + own_raised
    return (raised / total[..., None], own_raised / total)

def attend_block(tokens, lengths, cache_keys, cache_values, query_w, key_w, value_w, out_w, mix_lambda, head_gain, attn_gain, ffn_gain):
    rows = tokens.shape[0]
    groups = HEADS // KV_HEADS
    half = HEAD_DIM // 2
    scale = (HEAD_DIM // 2) ** (-0.5)
    xfull = tokens.astype(jnp.float32)
    normed = rms_norm(xfull, attn_gain, 1e-06).astype(jnp.bfloat16)
    query = jnp.dot(normed, query_w, preferred_element_type=jnp.float32).astype(jnp.bfloat16)
    key_new = jnp.dot(normed, key_w, preferred_element_type=jnp.float32).astype(jnp.bfloat16)
    value_new = jnp.dot(normed, value_w, preferred_element_type=jnp.float32).astype(jnp.bfloat16)
    qfull = query.astype(jnp.float32).reshape(rows, KV_HEADS, groups, HEAD_DIM)
    knew = key_new.astype(jnp.float32).reshape(rows, KV_HEADS, HEAD_DIM)
    vnew = value_new.astype(jnp.float32).reshape(rows, KV_HEADS, HEAD_DIM)
    kcache = cache_keys.astype(jnp.float32)
    vcache = cache_values.astype(jnp.float32)
    valid = (jnp.arange(CACHE, dtype=jnp.int32)[None, :] < lengths[:, None])[:, None, None, :]
    first = jnp.einsum('sgqd,spgd->sgqp', qfull[..., :half], kcache[..., :half]) * scale
    first_own = jnp.einsum('sgqd,sgd->sgq', qfull[..., :half], knew[..., :half]) * scale
    second = jnp.einsum('sgqd,spgd->sgqp', qfull[..., half:], kcache[..., half:]) * scale
    second_own = jnp.einsum('sgqd,sgd->sgq', qfull[..., half:], knew[..., half:]) * scale
    prob_one, own_one = softmax_pair(first, first_own, valid)
    prob_two, own_two = softmax_pair(second, second_own, valid)
    lam = mix_lambda.astype(jnp.float32).reshape(KV_HEADS, groups)
    weights = (prob_one - lam[None, :, :, None] * prob_two).astype(jnp.bfloat16)
    own_weights = (own_one - lam[None] * own_two).astype(jnp.bfloat16)
    mixed = jnp.einsum('sgqp,spgd->sgqd', weights.astype(jnp.float32), vcache)
    mixed = mixed + own_weights.astype(jnp.float32)[..., None] * vnew[:, :, None, :]
    heads = rms_norm(mixed, head_gain, 1e-05).astype(jnp.bfloat16).reshape(rows, HEADS * HEAD_DIM)
    hidden_state = xfull + jnp.dot(heads, out_w, preferred_element_type=jnp.float32)
    ffn_in = rms_norm(hidden_state, ffn_gain, 1e-06).astype(jnp.bfloat16)
    return (hidden_state, ffn_in, key_new, value_new)

def reference(tokens, lengths, cache_keys, cache_values, query_w, key_w, value_w, out_w, mix_lambda, head_gain, attn_gain, ffn_gain, routes, route_weights, exp_gate, exp_up, exp_down, dense_gate, dense_up, dense_down, branch_gate):
    blocks = tokens.shape[0] // SEQ_DEV

    def one_block(pieces):
        return attend_block(pieces[0], pieces[1], pieces[2], pieces[3], query_w, key_w, value_w, out_w, mix_lambda, head_gain, attn_gain, ffn_gain)
    hidden_state, ffn_in, key_new, value_new = lax.map(one_block, (tokens.reshape(blocks, SEQ_DEV, D), lengths.reshape(blocks, SEQ_DEV), cache_keys.reshape(blocks, SEQ_DEV, CACHE, KV_HEADS, HEAD_DIM), cache_values.reshape(blocks, SEQ_DEV, CACHE, KV_HEADS, HEAD_DIM)))
    hidden_state = hidden_state.reshape(TOKENS, D)
    ffn_in = ffn_in.reshape(TOKENS, D)
    key_new = key_new.reshape(TOKENS, KV_HEADS * HEAD_DIM)
    value_new = value_new.reshape(TOKENS, KV_HEADS * HEAD_DIM)
    slots = N_EP * CAP

    def one_expert(total, expert):
        match = routes == expert
        hit = jnp.any(match, axis=-1)
        weight = lax.optimization_barrier(jnp.sum(jnp.where(match, route_weights.astype(jnp.float32), 0.0), axis=-1))
        rank = jnp.cumsum(hit.astype(jnp.int32)) - 1
        select = hit[None, :] & (rank[None, :] == jnp.arange(slots, dtype=jnp.int32)[:, None])
        chosen = jnp.dot(select.astype(jnp.bfloat16), ffn_in, preferred_element_type=jnp.float32).astype(jnp.bfloat16)
        start = (expert * EXP_FF).astype(jnp.int32)
        w_gate = lax.dynamic_slice_in_dim(exp_gate, start, EXP_FF, 1)
        w_up = lax.dynamic_slice_in_dim(exp_up, start, EXP_FF, 1)
        w_down = lax.dynamic_slice_in_dim(exp_down, start, EXP_FF, 0)
        gate_part = jnp.dot(chosen, w_gate, preferred_element_type=jnp.float32)
        up_part = jnp.dot(chosen, w_up, preferred_element_type=jnp.float32)
        act = (jax.nn.silu(gate_part) * up_part).astype(jnp.bfloat16)
        result = jnp.dot(act, w_down, preferred_element_type=jnp.float32)
        back = jnp.dot(select.astype(jnp.float32).T, result, precision=lax.Precision.HIGHEST)
        return (total + weight[:, None] * back, None)
    routed, unused = lax.scan(one_expert, jnp.zeros((TOKENS, D), jnp.float32), jnp.arange(EXPERTS, dtype=jnp.int32))
    row_span = D // BLOCKS
    col_span = DENSE_FF // SPLIT
    gate_full = dense_gate.reshape(BLOCKS, SPLIT, row_span, col_span).transpose(0, 2, 1, 3).reshape(D, DENSE_FF)
    up_full = dense_up.reshape(BLOCKS, SPLIT, row_span, col_span).transpose(0, 2, 1, 3).reshape(D, DENSE_FF)
    down_full = dense_down.reshape(BLOCKS, SPLIT, col_span, row_span).transpose(1, 2, 0, 3).reshape(DENSE_FF, D)
    gate_part = jnp.dot(ffn_in, gate_full, preferred_element_type=jnp.float32)
    up_part = jnp.dot(ffn_in, up_full, preferred_element_type=jnp.float32)
    dense_act = (jax.nn.silu(gate_part) * up_part).astype(jnp.bfloat16)
    dense = jnp.dot(dense_act, down_full, preferred_element_type=jnp.float32)
    gate = jax.nn.sigmoid(jnp.dot(ffn_in, branch_gate, preferred_element_type=jnp.float32))
    output = (hidden_state + routed + gate[:, None] * dense).astype(jnp.bfloat16)
    return (output, key_new, value_new)
```

```python
import jax
import jax.numpy as jnp
from jax import lax
from jax.experimental import pallas as pl
from jax.experimental.pallas import tpu as pltpu
from jax.sharding import PartitionSpec as P

BF = jnp.bfloat16
F32 = jnp.float32
MESH = pl.DeviceIdType.MESH
ALL = slice(None)
D = 2048
META = 128
HID = 384
UNITS = 44
PAD = 48
PARTS = ((0, 768, "xyz"), (768, 640, "yzx"), (1408, 640, "zxy"))
STRIDE = {"x": 2, "y": 8, "z": 32}
NT = (((1,), (1,)), ((), ()))


def pick(**at):
    return tuple(at.get(axis, ALL) for axis in "zyx")


def to_col(row):
    n = row.shape[1]
    same = lax.broadcasted_iota(jnp.int32, (n, n), 0) == lax.broadcasted_iota(jnp.int32, (n, n), 1)
    return jnp.sum(jnp.where(same, jnp.broadcast_to(row, (n, n)), 0.0), axis=1, keepdims=True)


def kernel(
    tokens, lengths, keys, values, query_w, key_w, value_w, out_w, mix_lambda, head_gain,
    attn_gain, ffn_gain, routes, route_weights, exp_gate, exp_up, exp_down,
    dense_gate, dense_up, dense_down, branch_gate,
    out, new_keys, new_values,
    tok_v, len_v, k_v, v_v, wq_v, wk_v, wv_v, wo_v, lam_v, hg_v, ag_v, fg_v, rt_v, rw_v, bg_v,
    w1, w2, dgu, dg_v, du_v, dd_v, ds, qs, hs, xa, xf, act, pd, rs0, pf, sb1, rb1, sb2, rb2, sb3, rb3,
    load_sem, small_sem, w_sem, own_sem,
    ds_send, ds_recv, ag_send, ag_recv, dx_send, dx_recv, rd_send, rd_recv, rs_send, rs_recv,
):
    me = lax.axis_index("ep")
    core = lax.rem(me, 2)
    coord = {
        "x": lax.rem(lax.div(me, 2), 4),
        "y": lax.rem(lax.div(me, 8), 4),
        "z": lax.div(me, 32),
    }
    block = lax.div(me, 16)
    column = lax.rem(me, 16)
    partner = me + 1 - 2 * core

    def along(axis, k):
        there = lax.rem(coord[axis] + k, 4)
        return me + (there - coord[axis]) * STRIDE[axis], there

    barrier = pltpu.get_barrier_semaphore()
    friends = [partner]
    for axis in "xyz":
        for k in (1, 2, 3):
            friends.append(along(axis, k)[0])
    y_there = lax.rem(coord["y"] + 2, 4)
    for k in (1, 2, 3):
        z_there = lax.rem(coord["z"] + k, 4)
        friends.append(me + (z_there - coord["z"]) * 32 + (y_there - coord["y"]) * 8)
    for friend in friends:
        pl.semaphore_signal(barrier, inc=1, device_id=(friend,), device_id_type=MESH)

    def load(src, dst, sem):
        copy = pltpu.make_async_copy(src, dst, sem)
        copy.start()
        return copy

    small = [
        load(src, dst, small_sem.at[i])
        for i, (src, dst) in enumerate(
            (
                (tokens, tok_v), (attn_gain, ag_v), (dense_gate.at[0], dg_v), (dense_up.at[0], du_v),
                (dense_down.at[0], dd_v), (lengths, len_v), (mix_lambda, lam_v), (head_gain, hg_v),
                (ffn_gain, fg_v), (routes, rt_v), (route_weights, rw_v), (branch_gate, bg_v),
            )
        )
    ]
    step = D // 4
    qkv_loads = []
    for i in range(4):
        rows = pl.ds(i * step, step)
        qkv_loads.append(
            [
                load(query_w.at[rows], wq_v.at[rows], load_sem.at[3 * i]),
                load(key_w.at[rows], wk_v.at[rows], load_sem.at[3 * i + 1]),
                load(value_w.at[rows], wv_v.at[rows], load_sem.at[3 * i + 2]),
            ]
        )
    k_loads = [load(keys.at[s], k_v.at[s], load_sem.at[12 + s]) for s in range(4)]
    v_loads = [load(values.at[s], v_v.at[s], load_sem.at[16 + s]) for s in range(4)]
    o_load = load(out_w, wo_v, load_sem.at[20])
    w_loads = []
    for n in range(3):
        cols = pl.ds(n * 128, 128)
        w_loads.append(load(exp_gate.at[:, cols], w1.at[n, :, pl.ds(0, 128)], w_sem.at[2 * n]))
        w_loads.append(load(exp_up.at[:, cols], w1.at[n, :, pl.ds(128, 128)], w_sem.at[2 * n + 1]))
    w_loads.append(load(exp_down, w2.at[pl.ds(0, HID)], w_sem.at[6]))

    dgu[:, PAD:, :] = jnp.zeros((2, 128 - PAD, D), BF)
    w2[HID + PAD :, :] = jnp.zeros((128 - PAD, D), BF)
    row_i = lax.broadcasted_iota(jnp.int32, (PAD, 352), 0)
    col_i = lax.broadcasted_iota(jnp.int32, (PAD, 352), 1)
    for i in (2, 3, 4):
        small[i].wait()
    choose = jnp.concatenate(
        [
            jnp.where((col_i == row_i + UNITS * j) & (row_i < UNITS), 1.0, 0.0)
            for j in range(8)
        ],
        axis=0,
    ).astype(BF)
    ds[:, 0] = lax.dot_general(choose, dg_v[...], NT, preferred_element_type=F32).astype(BF).reshape(8, PAD, 256)
    ds[:, 1] = lax.dot_general(choose, du_v[...], NT, preferred_element_type=F32).astype(BF).reshape(8, PAD, 256)
    ds[:, 2] = jnp.dot(choose, dd_v[...], preferred_element_type=F32).astype(BF).reshape(8, PAD, 256)

    small[0].wait()
    small[1].wait()
    x = tok_v[...].astype(F32)
    normed = (x * lax.rsqrt(jnp.mean(x * x, axis=1, keepdims=True) + 1e-6) * ag_v[...]).astype(BF)

    pl.semaphore_wait(barrier, len(friends))
    own_cols = pl.ds(pl.multiple_of(block * 256, 256), 256)
    sent = []
    for k in range(1, 8):
        there = lax.rem(block + k, 8)
        for j, (src, dst) in enumerate(
            (
                (ds.at[there, pl.ds(0, 2)], dgu.at[:, pl.ds(0, PAD), own_cols]),
                (ds.at[there, 2], w2.at[pl.ds(HID, PAD), own_cols]),
            )
        ):
            copy = pltpu.make_async_remote_copy(
                src_ref=src, dst_ref=dst, send_sem=ds_send.at[j, k - 1], recv_sem=ds_recv.at[j, k - 1],
                device_id=(there * 16 + column,), device_id_type=MESH,
            )
            copy.start()
            sent.append(copy)
    own_loads = [
        load(ds.at[block, pl.ds(0, 2)], dgu.at[:, pl.ds(0, PAD), own_cols], own_sem.at[0]),
        load(ds.at[block, 2], w2.at[pl.ds(HID, PAD), own_cols], own_sem.at[1]),
    ]

    query = jnp.zeros((4, 1024), F32)
    key = jnp.zeros((4, 256), F32)
    value = jnp.zeros((4, 256), F32)
    for i in range(4):
        for copy in qkv_loads[i]:
            copy.wait()
        part = normed[:, i * step : (i + 1) * step]
        rows = pl.ds(i * step, step)
        query += jnp.dot(part, wq_v[rows, :], preferred_element_type=F32)
        key += jnp.dot(part, wk_v[rows, :], preferred_element_type=F32)
        value += jnp.dot(part, wv_v[rows, :], preferred_element_type=F32)
    key = key.astype(BF)
    value = value.astype(BF)
    new_keys[...] = key
    new_values[...] = value
    key = key.astype(F32)
    value = value.astype(F32)
    query = query.astype(BF).astype(F32)
    for h in range(8):
        qs[h] = query[:, h * 128 : (h + 1) * 128]

    for i in range(5, 12):
        small[i].wait()
    lam = to_col(lam_v[...])
    row8 = lax.broadcasted_iota(jnp.int32, (8, 128), 0)
    lane8 = lax.broadcasted_iota(jnp.int32, (8, 128), 1)
    row16 = lax.rem(lax.broadcasted_iota(jnp.int32, (16, 2048), 0), 8)
    spot = lax.broadcasted_iota(jnp.int32, (16, 2048), 1)
    matching = lax.rem(spot, 2) == lax.div(row16, 4)
    for s in range(4):
        heads_q = qs[:, s, :]
        q16 = jnp.concatenate(
            [jnp.where(lane8 < 64, heads_q, 0.0), jnp.where(lane8 >= 64, heads_q, 0.0)], axis=0
        )
        own_key = jnp.where(row8 < 4, key[s : s + 1, :128], key[s : s + 1, 128:])
        own_value = jnp.where(row8 < 4, value[s : s + 1, :128], value[s : s + 1, 128:])
        k_loads[s].wait()
        scores = lax.dot_general(q16.astype(BF), k_v[s], NT, preferred_element_type=F32) * 0.125
        own = jnp.sum(q16 * jnp.concatenate([own_key, own_key], axis=0), axis=1, keepdims=True) * 0.125
        valid = matching & (spot < 2 * len_v[0:1, s : s + 1])
        largest = jnp.maximum(jnp.max(jnp.where(valid, scores, -jnp.inf), axis=1, keepdims=True), own)
        raised = jnp.where(valid, jnp.exp(scores - largest), 0.0)
        own_raised = jnp.exp(own - largest)
        total = jnp.sum(raised, axis=1, keepdims=True) + own_raised
        prob = raised / total
        own_prob = own_raised / total
        weights = (prob[:8] - lam * prob[8:]).astype(BF)
        own_weight = (own_prob[:8] - lam * own_prob[8:]).astype(BF).astype(F32)
        v_loads[s].wait()
        mixed = jnp.dot(weights, v_v[s], preferred_element_type=F32) + own_weight * own_value
        mixed = mixed * lax.rsqrt(jnp.mean(mixed * mixed, axis=1, keepdims=True) + 1e-5) * hg_v[...]
        hs[s] = mixed
    heads = jnp.concatenate([hs[:, h, :] for h in range(8)], axis=1).astype(BF)
    o_load.wait()
    hidden = x + jnp.dot(heads, wo_v[...], preferred_element_type=F32)
    ffn_in = (
        hidden * lax.rsqrt(jnp.mean(hidden * hidden, axis=1, keepdims=True) + 1e-6) * fg_v[...]
    ).astype(BF)
    gate = jax.nn.sigmoid(
        jnp.sum(ffn_in.astype(F32) * bg_v[...].astype(F32), axis=1, keepdims=True)
    )
    lane4 = lax.broadcasted_iota(jnp.int32, (4, META), 1)
    expert4 = lax.rem(lane4, 8)
    scale = jnp.where(lane4 < 16, 0.0, gate)
    for j in range(2):
        named = to_col(rt_v[j : j + 1, :].astype(F32)).astype(jnp.int32)
        scale += jnp.where((expert4 == named) & (lane4 < 16), to_col(rw_v[j : j + 1, :]), 0.0)
    upper = scale.astype(BF).astype(F32)
    meta = jnp.where(
        (lane4 < 8) | (lane4 == 16), upper, jnp.where((lane4 < 16) | (lane4 == 17), scale - upper, 0.0)
    ).astype(BF)
    mine = (coord["z"], coord["y"], coord["x"])
    xa[(core,) + mine] = jnp.concatenate([ffn_in, meta], axis=1)

    def width(p):
        off, n, order = PARTS[p]
        return pl.ds(off, n + META if p == 2 else n)

    def moved(p, phase, k, at, to, sems):
        send, recv = sems
        ref = xa.at[(core,) + at + (ALL, width(p))]
        return pltpu.make_async_remote_copy(
            src_ref=ref, dst_ref=ref, send_sem=send.at[p, phase, k], recv_sem=recv.at[p, phase, k],
            device_id=(to,), device_id_type=MESH,
        )

    def over(p, k, at, half):
        ref = xa.at[(half,) + at + (ALL, width(p))]
        return pltpu.make_async_remote_copy(
            src_ref=ref, dst_ref=ref, send_sem=dx_send.at[p, k], recv_sem=dx_recv.at[p, k],
            device_id=(partner,), device_id_type=MESH,
        )

    arrivals = {}
    for phase in range(3):
        for p in range(3):
            order = PARTS[p][2]
            if phase > 0:
                for copy in arrivals[p, phase - 1]:
                    copy.wait_recv()
            fixed = {axis: coord[axis] for axis in order[phase:]}
            axis = order[phase]
            arrivals[p, phase] = []
            for k in (1, 2, 3):
                to, there = along(axis, k)
                copy = moved(p, phase, k - 1, pick(**fixed), to, (ag_send, ag_recv))
                copy.start()
                sent.append(copy)
                back = lax.rem(coord[axis] + 4 - k, 4)
                arrivals[p, phase].append(
                    moved(p, phase, k - 1, pick(**{**fixed, axis: back}), to, (ag_send, ag_recv))
                )
            if phase == 2:
                copy = over(p, 0, pick(**fixed), core)
                copy.start()
                sent.append(copy)
    for k in (1, 2, 3):
        for p in range(3):
            axis = PARTS[p][2][2]
            arrivals[p, 2][k - 1].wait_recv()
            back = lax.rem(coord[axis] + 4 - k, 4)
            copy = over(p, k, pick(**{axis: back}), core)
            copy.start()
            sent.append(copy)

    def settle(half):
        def body(z, carry):
            rows = pl.ds(pl.multiple_of(z * 64, 64), 64)
            xf[half, rows, :] = xa[half, z].reshape(64, D + META)
            return carry

        lax.fori_loop(0, 4, body, 0)

    settle(core)
    for p in range(3):
        axis = PARTS[p][2][2]
        for k in range(4):
            back = lax.rem(coord[axis] + 4 - k, 4)
            over(p, k, pick(**{axis: back}), 1 - core).wait_recv()
    settle(1 - core)

    lane = lax.broadcasted_iota(jnp.int32, (512, META), 1)
    scales = xf[:, :, D:].reshape(512, META).astype(F32)
    route = jnp.sum(jnp.where((lane == block) | (lane == block + 8), scales, 0.0), axis=1, keepdims=True)
    dense = jnp.sum(jnp.where((lane == 16) | (lane == 17), scales, 0.0), axis=1, keepdims=True)
    for copy in w_loads:
        copy.wait()

    def expert(n, carry):
        both = jnp.dot(xf[:, :, :D].reshape(512, D), w1[n], preferred_element_type=F32)
        g, u = both[:, :128], both[:, 128:]
        act[n] = (g * jax.nn.sigmoid(g) * u * route).astype(BF)
        return carry

    lax.fori_loop(0, 3, expert, 0)
    for copy in own_loads:
        copy.wait()
    for k in range(1, 8):
        back = lax.rem(block + 8 - k, 8)
        cols = pl.ds(pl.multiple_of(back * 256, 256), 256)
        for j, (src, dst) in enumerate(
            (
                (ds.at[block, pl.ds(0, 2)], dgu.at[:, pl.ds(0, PAD), cols]),
                (ds.at[block, 2], w2.at[pl.ds(HID, PAD), cols]),
            )
        ):
            pltpu.make_async_remote_copy(
                src_ref=src, dst_ref=dst, send_sem=ds_send.at[j, k - 1], recv_sem=ds_recv.at[j, k - 1],
                device_id=(back * 16 + column,), device_id_type=MESH,
            ).wait_recv()
    both = lax.dot_general(xf[:, :, :D].reshape(512, D), dgu[...].reshape(256, D), NT, preferred_element_type=F32)
    g, u = both[:, :128], both[:, 128:]
    act[3] = (g * jax.nn.sigmoid(g) * u * dense).astype(BF)

    def columns(p):
        return pl.ds(PARTS[p][0], PARTS[p][1])

    def product(half, p):
        rows = pl.ds(pl.multiple_of(half * 256, 256), 256)
        left = jnp.concatenate([act[n, rows, :] for n in range(4)], axis=1)
        return jnp.dot(left, w2[:, columns(p)], preferred_element_type=F32)

    def swap(p):
        at = (ALL, ALL, ALL, ALL, columns(p))
        return pltpu.make_async_remote_copy(
            src_ref=pd.at[at], dst_ref=rs0.at[at], send_sem=rd_send.at[p], recv_sem=rd_recv.at[p],
            device_id=(partner,), device_id_type=MESH,
        )

    def multiply(p):
        n = PARTS[p][1]
        pd[:, :, :, :, columns(p)] = product(1 - core, p).astype(BF).reshape(4, 4, 4, 4, n)
        copy = swap(p)
        copy.start()
        sent.append(copy)
        pf[:, columns(p)] = product(core, p)

    def hop(p, phase):
        axis = PARTS[p][2][2 - phase]
        copies = []
        for k in (1, 2, 3):
            to, there = along(axis, k)
            if phase == 0:
                src = sb1.at[pick(**{axis: there}) + (ALL, columns(p))]
                dst = rb1.at[k - 1, :, :, :, columns(p)]
            elif phase == 1:
                order = PARTS[p][2]
                first = "zyx".index(order[1]) < "zyx".index(order[0])
                at = (there, ALL) if first else (ALL, there)
                src = sb2.at[at + (ALL, columns(p))]
                dst = rb2.at[k - 1, :, :, columns(p)]
            else:
                src = sb3.at[there, :, columns(p)]
                dst = rb3.at[k - 1, :, columns(p)]
            copy = pltpu.make_async_remote_copy(
                src_ref=src, dst_ref=dst, send_sem=rs_send.at[p, phase, k - 1], recv_sem=rs_recv.at[p, phase, k - 1],
                device_id=(to,), device_id_type=MESH,
            )
            copy.start()
            copies.append(copy)
            sent.append(copy)
        return copies

    flights = {}

    def begin(p):
        n = PARTS[p][1]
        swap(p).wait_recv()
        far = rs0[:, :, :, :, columns(p)].reshape(256, n).astype(F32)
        sb1[:, :, :, :, columns(p)] = (pf[:, columns(p)] + far).astype(BF).reshape(4, 4, 4, 4, n)
        flights[p] = hop(p, 0)

    multiply(0)
    multiply(1)
    begin(0)
    multiply(2)
    begin(1)
    begin(2)
    for p in range(3):
        n = PARTS[p][1]
        axis = PARTS[p][2][2]
        for copy in flights[p]:
            copy.wait_recv()
        total = sb1[pick(**{axis: coord[axis]}) + (ALL, columns(p))].reshape(64, n).astype(F32)
        for k in range(3):
            total += rb1[k, :, :, :, columns(p)].reshape(64, n).astype(F32)
        sb2[:, :, :, columns(p)] = total.astype(BF).reshape(4, 4, 4, n)
        flights[p] = hop(p, 1)
    for p in range(3):
        n = PARTS[p][1]
        order = PARTS[p][2]
        for copy in flights[p]:
            copy.wait_recv()
        first = "zyx".index(order[1]) < "zyx".index(order[0])
        at = (coord[order[1]], ALL) if first else (ALL, coord[order[1]])
        total = sb2[at + (ALL, columns(p))].reshape(16, n).astype(F32)
        for k in range(3):
            total += rb2[k, :, :, columns(p)].reshape(16, n).astype(F32)
        sb3[:, :, columns(p)] = total.astype(BF).reshape(4, 4, n)
        flights[p] = hop(p, 2)
    for p in range(3):
        off, n, order = PARTS[p]
        for copy in flights[p]:
            copy.wait_recv()
        total = sb3[coord[order[0]], :, columns(p)].astype(F32)
        for k in range(3):
            total += rb3[k, :, columns(p)].astype(F32)
        out[:, off : off + n] = (hidden[:, off : off + n] + total).astype(BF)
    for copy in sent:
        copy.wait_send()


def per_device(
    tokens, lengths, cache_keys, cache_values, query_w, key_w, value_w, out_w, mix_lambda, head_gain,
    attn_gain, ffn_gain, routes, route_weights, exp_gate, exp_up, exp_down,
    dense_gate, dense_up, dense_down, branch_gate,
):
    def vm(*shape, dtype=BF):
        return pltpu.VMEM(shape, dtype)

    dma = pltpu.SemaphoreType.DMA
    scratch = [
        vm(4, D), vm(1, 4, dtype=jnp.int32), vm(4, 2048, 128), vm(4, 2048, 128),
        vm(D, 1024), vm(D, 256), vm(D, 256), vm(1024, D),
        vm(1, 8, dtype=F32), vm(1, 128, dtype=F32), vm(1, D, dtype=F32), vm(1, D, dtype=F32),
        vm(2, 4, dtype=jnp.int32), vm(2, 4, dtype=F32), vm(1, D),
        vm(3, D, 256), vm(512, D), vm(2, 128, D), vm(256, 352), vm(256, 352), vm(352, 256),
        vm(8, 3, PAD, 256), vm(8, 4, 128, dtype=F32), vm(4, 8, 128, dtype=F32),
        vm(2, 4, 4, 4, 4, D + META), vm(2, 256, D + META), vm(4, 512, 128),
        vm(4, 4, 4, 4, D), vm(4, 4, 4, 4, D), vm(256, D, dtype=F32), vm(4, 4, 4, 4, D),
        vm(3, 4, 4, 4, D), vm(4, 4, 4, D), vm(3, 4, 4, D), vm(4, 4, D), vm(3, 4, D),
        dma((21,)), dma((12,)), dma((7,)), dma((2,)),
        dma((2, 7)), dma((2, 7)), dma((3, 3, 3)), dma((3, 3, 3)), dma((3, 4)), dma((3, 4)),
        dma((3,)), dma((3,)), dma((3, 3, 3)), dma((3, 3, 3)),
    ]
    return pl.pallas_call(
        kernel,
        out_shape=(
            jax.ShapeDtypeStruct((4, D), BF),
            jax.ShapeDtypeStruct((4, 256), BF),
            jax.ShapeDtypeStruct((4, 256), BF),
        ),
        in_specs=[pl.BlockSpec(memory_space=pl.ANY)] * 21,
        out_specs=[pl.BlockSpec(memory_space=pltpu.VMEM)] * 3,
        scratch_shapes=scratch,
        compiler_params=pltpu.CompilerParams(
            collective_id=0, has_side_effects=True, vmem_limit_bytes=56 * 1024 * 1024
        ),
        name="layer",
    )(
        tokens, lengths.reshape(1, 4), cache_keys.reshape(4, 2048, 128), cache_values.reshape(4, 2048, 128),
        query_w, key_w, value_w, out_w, mix_lambda.reshape(1, 8), head_gain.reshape(1, 128),
        attn_gain.reshape(1, D), ffn_gain.reshape(1, D), routes.T, route_weights.T,
        exp_gate, exp_up, exp_down, dense_gate, dense_up, dense_down, branch_gate.reshape(1, D),
    )


def solution(mesh):
    placed = (
        P("ep", None), P("ep"), P("ep", None, None, None), P("ep", None, None, None),
        P(), P(), P(), P(), P(), P(), P(), P(),
        P("ep", None), P("ep", None), P(None, "ep"), P(None, "ep"), P("ep", None),
        P("ep", None, None), P("ep", None, None), P("ep", None, None), P(),
    )
    return jax.shard_map(
        per_device,
        mesh=mesh,
        in_specs=placed,
        out_specs=(P("ep", None), P("ep", None), P("ep", None)),
        check_vma=False,
    )
```

```python
import jax
import jax.numpy as jnp
from jax import lax
from jax.experimental import pallas as pl
from jax.experimental.pallas import tpu as pltpu
from jax.sharding import PartitionSpec as P

BF = jnp.bfloat16
F32 = jnp.float32
MESH = pl.DeviceIdType.MESH
ALL = slice(None)
D = 2048
META = 128
HID = 384
UNITS = 44
PAD = 48
PARTS = ((0, 768, "xyz"), (768, 640, "yzx"), (1408, 640, "zxy"))
STRIDE = {"x": 2, "y": 8, "z": 32}
NT = (((1,), (1,)), ((), ()))


def pick(**at):
    return tuple(at.get(axis, ALL) for axis in "zyx")


def to_col(row):
    n = row.shape[1]
    same = lax.broadcasted_iota(jnp.int32, (n, n), 0) == lax.broadcasted_iota(jnp.int32, (n, n), 1)
    return jnp.sum(jnp.where(same, jnp.broadcast_to(row, (n, n)), 0.0), axis=1, keepdims=True)


def kernel(
    tokens, lengths, keys, values, query_w, key_w, value_w, out_w, mix_lambda, head_gain,
    attn_gain, ffn_gain, routes, route_weights, exp_gate, exp_up, exp_down,
    dense_gate, dense_up, dense_down, branch_gate,
    out, new_keys, new_values,
    tok_v, len_v, k_v, v_v, wq_v, wk_v, wv_v, wo_v, lam_v, hg_v, ag_v, fg_v, rt_v, rw_v, bg_v,
    w1, w2, dgu, dg_v, du_v, dd_v, ds, qs, hs, xa, xf, act, pd, rs0, pf, sb1, rb1, sb2, rb2, sb3, rb3,
    load_sem, small_sem, w_sem, own_sem,
    ds_send, ds_recv, ag_send, ag_recv, dx_send, dx_recv, rd_send, rd_recv, rs_send, rs_recv,
):
    me = lax.axis_index("ep")
    core = lax.rem(me, 2)
    coord = {
        "x": lax.rem(lax.div(me, 2), 4),
        "y": lax.rem(lax.div(me, 8), 4),
        "z": lax.div(me, 32),
    }
    block = lax.div(me, 16)
    column = lax.rem(me, 16)
    partner = me + 1 - 2 * core

    def along(axis, k):
        there = lax.rem(coord[axis] + k, 4)
        return me + (there - coord[axis]) * STRIDE[axis], there

    barrier = pltpu.get_barrier_semaphore()
    friends = [partner]
    for axis in "xyz":
        for k in (1, 2, 3):
            friends.append(along(axis, k)[0])
    y_there = lax.rem(coord["y"] + 2, 4)
    for k in (1, 2, 3):
        z_there = lax.rem(coord["z"] + k, 4)
        friends.append(me + (z_there - coord["z"]) * 32 + (y_there - coord["y"]) * 8)
    for friend in friends:
        pl.semaphore_signal(barrier, inc=1, device_id=(friend,), device_id_type=MESH)

    def load(src, dst, sem):
        copy = pltpu.make_async_copy(src, dst, sem)
        copy.start()
        return copy

    small = [
        load(src, dst, small_sem.at[i])
        for i, (src, dst) in enumerate(
            (
                (tokens, tok_v), (attn_gain, ag_v), (dense_gate.at[0], dg_v), (dense_up.at[0], du_v),
                (dense_down.at[0], dd_v), (lengths, len_v), (mix_lambda, lam_v), (head_gain, hg_v),
                (ffn_gain, fg_v), (routes, rt_v), (route_weights, rw_v), (branch_gate, bg_v),
            )
        )
    ]
    step = D // 4
    qkv_loads = []
    for i in range(4):
        rows = pl.ds(i * step, step)
        qkv_loads.append(
            [
                load(query_w.at[rows], wq_v.at[rows], load_sem.at[3 * i]),
                load(key_w.at[rows], wk_v.at[rows], load_sem.at[3 * i + 1]),
                load(value_w.at[rows], wv_v.at[rows], load_sem.at[3 * i + 2]),
            ]
        )
    k_loads = [load(keys.at[s], k_v.at[s], load_sem.at[12 + s]) for s in range(4)]
    v_loads = [load(values.at[s], v_v.at[s], load_sem.at[16 + s]) for s in range(4)]
    o_load = load(out_w, wo_v, load_sem.at[20])
    w_loads = []
    for n in range(3):
        cols = pl.ds(n * 128, 128)
        w_loads.append(load(exp_gate.at[:, cols], w1.at[n, :, pl.ds(0, 128)], w_sem.at[2 * n]))
        w_loads.append(load(exp_up.at[:, cols], w1.at[n, :, pl.ds(128, 128)], w_sem.at[2 * n + 1]))
    w_loads.append(load(exp_down, w2.at[pl.ds(0, HID)], w_sem.at[6]))

    dgu[:, PAD:, :] = jnp.zeros((2, 128 - PAD, D), BF)
    w2[HID + PAD :, :] = jnp.zeros((128 - PAD, D), BF)
    row_i = lax.broadcasted_iota(jnp.int32, (PAD, 352), 0)
    col_i = lax.broadcasted_iota(jnp.int32, (PAD, 352), 1)
    for i in (2, 3, 4):
        small[i].wait()
    choose = jnp.concatenate(
        [
            jnp.where((col_i == row_i + UNITS * j) & (row_i < UNITS), 1.0, 0.0)
            for j in range(8)
        ],
        axis=0,
    ).astype(BF)
    for j, tile in enumerate((dg_v, du_v, dd_v)):
        ds[:, j] = jnp.dot(choose, tile[...], preferred_element_type=F32).astype(BF).reshape(8, PAD, 256)

    small[0].wait()
    small[1].wait()
    x = tok_v[...].astype(F32)
    normed = (x * lax.rsqrt(jnp.mean(x * x, axis=1, keepdims=True) + 1e-6) * ag_v[...]).astype(BF)

    pl.semaphore_wait(barrier, len(friends))
    own_cols = pl.ds(pl.multiple_of(block * 256, 256), 256)
    sent = []
    for k in range(1, 8):
        there = lax.rem(block + k, 8)
        for j, (src, dst) in enumerate(
            (
                (ds.at[there, pl.ds(0, 2)], dgu.at[:, pl.ds(0, PAD), own_cols]),
                (ds.at[there, 2], w2.at[pl.ds(HID, PAD), own_cols]),
            )
        ):
            copy = pltpu.make_async_remote_copy(
                src_ref=src, dst_ref=dst, send_sem=ds_send.at[j, k - 1], recv_sem=ds_recv.at[j, k - 1],
                device_id=(there * 16 + column,), device_id_type=MESH,
            )
            copy.start()
            sent.append(copy)
    own_loads = [
        load(ds.at[block, pl.ds(0, 2)], dgu.at[:, pl.ds(0, PAD), own_cols], own_sem.at[0]),
        load(ds.at[block, 2], w2.at[pl.ds(HID, PAD), own_cols], own_sem.at[1]),
    ]

    query = jnp.zeros((4, 1024), F32)
    key = jnp.zeros((4, 256), F32)
    value = jnp.zeros((4, 256), F32)
    for i in range(4):
        for copy in qkv_loads[i]:
            copy.wait()
        part = normed[:, i * step : (i + 1) * step]
        rows = pl.ds(i * step, step)
        query += jnp.dot(part, wq_v[rows, :], preferred_element_type=F32)
        key += jnp.dot(part, wk_v[rows, :], preferred_element_type=F32)
        value += jnp.dot(part, wv_v[rows, :], preferred_element_type=F32)
    key = key.astype(BF)
    value = value.astype(BF)
    new_keys[...] = key
    new_values[...] = value
    key = key.astype(F32)
    value = value.astype(F32)
    query = query.astype(BF).astype(F32)
    for h in range(8):
        qs[h] = query[:, h * 128 : (h + 1) * 128]

    for i in range(5, 12):
        small[i].wait()
    lam = to_col(lam_v[...])
    row8 = lax.broadcasted_iota(jnp.int32, (8, 128), 0)
    lane8 = lax.broadcasted_iota(jnp.int32, (8, 128), 1)
    row16 = lax.rem(lax.broadcasted_iota(jnp.int32, (16, 2048), 0), 8)
    spot = lax.broadcasted_iota(jnp.int32, (16, 2048), 1)
    matching = lax.rem(spot, 2) == lax.div(row16, 4)
    for s in range(4):
        heads_q = qs[:, s, :]
        q16 = jnp.concatenate(
            [jnp.where(lane8 < 64, heads_q, 0.0), jnp.where(lane8 >= 64, heads_q, 0.0)], axis=0
        )
        own_key = jnp.where(row8 < 4, key[s : s + 1, :128], key[s : s + 1, 128:])
        own_value = jnp.where(row8 < 4, value[s : s + 1, :128], value[s : s + 1, 128:])
        k_loads[s].wait()
        scores = lax.dot_general(q16.astype(BF), k_v[s], NT, preferred_element_type=F32) * 0.125
        own = jnp.sum(q16 * jnp.concatenate([own_key, own_key], axis=0), axis=1, keepdims=True) * 0.125
        valid = matching & (spot < 2 * len_v[0:1, s : s + 1])
        largest = jnp.maximum(jnp.max(jnp.where(valid, scores, -jnp.inf), axis=1, keepdims=True), own)
        raised = jnp.where(valid, jnp.exp(scores - largest), 0.0)
        own_raised = jnp.exp(own - largest)
        total = jnp.sum(raised, axis=1, keepdims=True) + own_raised
        prob = raised / total
        own_prob = own_raised / total
        weights = (prob[:8] - lam * prob[8:]).astype(BF)
        own_weight = (own_prob[:8] - lam * own_prob[8:]).astype(BF).astype(F32)
        v_loads[s].wait()
        mixed = jnp.dot(weights, v_v[s], preferred_element_type=F32) + own_weight * own_value
        mixed = mixed * lax.rsqrt(jnp.mean(mixed * mixed, axis=1, keepdims=True) + 1e-5) * hg_v[...]
        hs[s] = mixed
    heads = jnp.concatenate([hs[:, h, :] for h in range(8)], axis=1).astype(BF)
    o_load.wait()
    hidden = x + jnp.dot(heads, wo_v[...], preferred_element_type=F32)
    ffn_in = (
        hidden * lax.rsqrt(jnp.mean(hidden * hidden, axis=1, keepdims=True) + 1e-6) * fg_v[...]
    ).astype(BF)
    gate_w = bg_v[...].astype(F32)
    toward = jnp.zeros((4, 128), F32)
    for j in range(16):
        toward += ffn_in[:, j * 128 : (j + 1) * 128].astype(F32) * gate_w[j : j + 1]
    gate = jax.nn.sigmoid(jnp.sum(toward, axis=1, keepdims=True))
    lane4 = lax.broadcasted_iota(jnp.int32, (4, META), 1)
    expert4 = lax.rem(lane4, 8)
    scale = jnp.where(lane4 < 16, 0.0, gate)
    for j in range(2):
        named = to_col(rt_v[j : j + 1, :].astype(F32)).astype(jnp.int32)
        scale += jnp.where((expert4 == named) & (lane4 < 16), to_col(rw_v[j : j + 1, :]), 0.0)
    upper = scale.astype(BF).astype(F32)
    meta = jnp.where(
        (lane4 < 8) | (lane4 == 16), upper, jnp.where((lane4 < 16) | (lane4 == 17), scale - upper, 0.0)
    ).astype(BF)
    mine = (coord["z"], coord["y"], coord["x"])
    xa[(core,) + mine] = jnp.concatenate([ffn_in, meta], axis=1)

    def width(p):
        off, n, order = PARTS[p]
        return pl.ds(off, n + META if p == 2 else n)

    def moved(p, phase, k, at, to, sems):
        send, recv = sems
        ref = xa.at[(core,) + at + (ALL, width(p))]
        return pltpu.make_async_remote_copy(
            src_ref=ref, dst_ref=ref, send_sem=send.at[p, phase, k], recv_sem=recv.at[p, phase, k],
            device_id=(to,), device_id_type=MESH,
        )

    def over(p, k, at, half):
        ref = xa.at[(half,) + at + (ALL, width(p))]
        return pltpu.make_async_remote_copy(
            src_ref=ref, dst_ref=ref, send_sem=dx_send.at[p, k], recv_sem=dx_recv.at[p, k],
            device_id=(partner,), device_id_type=MESH,
        )

    arrivals = {}
    for phase in range(3):
        for p in range(3):
            order = PARTS[p][2]
            if phase > 0:
                for copy in arrivals[p, phase - 1]:
                    copy.wait_recv()
            fixed = {axis: coord[axis] for axis in order[phase:]}
            axis = order[phase]
            arrivals[p, phase] = []
            for k in (1, 2, 3):
                to, there = along(axis, k)
                copy = moved(p, phase, k - 1, pick(**fixed), to, (ag_send, ag_recv))
                copy.start()
                sent.append(copy)
                back = lax.rem(coord[axis] + 4 - k, 4)
                arrivals[p, phase].append(
                    moved(p, phase, k - 1, pick(**{**fixed, axis: back}), to, (ag_send, ag_recv))
                )
            if phase == 2:
                copy = over(p, 0, pick(**fixed), core)
                copy.start()
                sent.append(copy)
    for k in (1, 2, 3):
        for p in range(3):
            axis = PARTS[p][2][2]
            arrivals[p, 2][k - 1].wait_recv()
            back = lax.rem(coord[axis] + 4 - k, 4)
            copy = over(p, k, pick(**{axis: back}), core)
            copy.start()
            sent.append(copy)

    def settle(half):
        def body(z, carry):
            rows = pl.ds(pl.multiple_of(z * 64, 64), 64)
            xf[half, rows, :] = xa[half, z].reshape(64, D + META)
            return carry

        lax.fori_loop(0, 4, body, 0)

    settle(core)
    for p in range(3):
        axis = PARTS[p][2][2]
        for k in range(4):
            back = lax.rem(coord[axis] + 4 - k, 4)
            over(p, k, pick(**{axis: back}), 1 - core).wait_recv()
    settle(1 - core)

    lane = lax.broadcasted_iota(jnp.int32, (512, META), 1)
    scales = xf[:, :, D:].reshape(512, META).astype(F32)
    route = jnp.sum(jnp.where((lane == block) | (lane == block + 8), scales, 0.0), axis=1, keepdims=True)
    dense = jnp.sum(jnp.where((lane == 16) | (lane == 17), scales, 0.0), axis=1, keepdims=True)
    for copy in w_loads:
        copy.wait()

    def expert(n, carry):
        both = jnp.dot(xf[:, :, :D].reshape(512, D), w1[n], preferred_element_type=F32)
        g, u = both[:, :128], both[:, 128:]
        act[n] = (g * jax.nn.sigmoid(g) * u * route).astype(BF)
        return carry

    lax.fori_loop(0, 3, expert, 0)
    for copy in own_loads:
        copy.wait()
    for k in range(1, 8):
        back = lax.rem(block + 8 - k, 8)
        cols = pl.ds(pl.multiple_of(back * 256, 256), 256)
        for j, (src, dst) in enumerate(
            (
                (ds.at[block, pl.ds(0, 2)], dgu.at[:, pl.ds(0, PAD), cols]),
                (ds.at[block, 2], w2.at[pl.ds(HID, PAD), cols]),
            )
        ):
            pltpu.make_async_remote_copy(
                src_ref=src, dst_ref=dst, send_sem=ds_send.at[j, k - 1], recv_sem=ds_recv.at[j, k - 1],
                device_id=(back * 16 + column,), device_id_type=MESH,
            ).wait_recv()
    both = lax.dot_general(xf[:, :, :D].reshape(512, D), dgu[...].reshape(256, D), NT, preferred_element_type=F32)
    g, u = both[:, :128], both[:, 128:]
    act[3] = (g * jax.nn.sigmoid(g) * u * dense).astype(BF)

    def columns(p):
        return pl.ds(PARTS[p][0], PARTS[p][1])

    def product(half, p):
        rows = pl.ds(pl.multiple_of(half * 256, 256), 256)
        left = jnp.concatenate([act[n, rows, :] for n in range(4)], axis=1)
        return jnp.dot(left, w2[:, columns(p)], preferred_element_type=F32)

    def swap(p):
        at = (ALL, ALL, ALL, ALL, columns(p))
        return pltpu.make_async_remote_copy(
            src_ref=pd.at[at], dst_ref=rs0.at[at], send_sem=rd_send.at[p], recv_sem=rd_recv.at[p],
            device_id=(partner,), device_id_type=MESH,
        )

    def multiply(p):
        n = PARTS[p][1]
        pd[:, :, :, :, columns(p)] = product(1 - core, p).astype(BF).reshape(4, 4, 4, 4, n)
        copy = swap(p)
        copy.start()
        sent.append(copy)
        pf[:, columns(p)] = product(core, p)

    def hop(p, phase):
        axis = PARTS[p][2][2 - phase]
        copies = []
        for k in (1, 2, 3):
            to, there = along(axis, k)
            if phase == 0:
                src = sb1.at[pick(**{axis: there}) + (ALL, columns(p))]
                dst = rb1.at[k - 1, :, :, :, columns(p)]
            elif phase == 1:
                order = PARTS[p][2]
                first = "zyx".index(order[1]) < "zyx".index(order[0])
                at = (there, ALL) if first else (ALL, there)
                src = sb2.at[at + (ALL, columns(p))]
                dst = rb2.at[k - 1, :, :, columns(p)]
            else:
                src = sb3.at[there, :, columns(p)]
                dst = rb3.at[k - 1, :, columns(p)]
            copy = pltpu.make_async_remote_copy(
                src_ref=src, dst_ref=dst, send_sem=rs_send.at[p, phase, k - 1], recv_sem=rs_recv.at[p, phase, k - 1],
                device_id=(to,), device_id_type=MESH,
            )
            copy.start()
            copies.append(copy)
            sent.append(copy)
        return copies

    flights = {}

    def begin(p):
        n = PARTS[p][1]
        swap(p).wait_recv()
        far = rs0[:, :, :, :, columns(p)].reshape(256, n).astype(F32)
        sb1[:, :, :, :, columns(p)] = (pf[:, columns(p)] + far).astype(BF).reshape(4, 4, 4, 4, n)
        flights[p] = hop(p, 0)

    multiply(0)
    multiply(1)
    begin(0)
    multiply(2)
    begin(1)
    begin(2)
    for p in range(3):
        n = PARTS[p][1]
        axis = PARTS[p][2][2]
        for copy in flights[p]:
            copy.wait_recv()
        total = sb1[pick(**{axis: coord[axis]}) + (ALL, columns(p))].reshape(64, n).astype(F32)
        for k in range(3):
            total += rb1[k, :, :, :, columns(p)].reshape(64, n).astype(F32)
        sb2[:, :, :, columns(p)] = total.astype(BF).reshape(4, 4, 4, n)
        flights[p] = hop(p, 1)
    for p in range(3):
        n = PARTS[p][1]
        order = PARTS[p][2]
        for copy in flights[p]:
            copy.wait_recv()
        first = "zyx".index(order[1]) < "zyx".index(order[0])
        at = (coord[order[1]], ALL) if first else (ALL, coord[order[1]])
        total = sb2[at + (ALL, columns(p))].reshape(16, n).astype(F32)
        for k in range(3):
            total += rb2[k, :, :, columns(p)].reshape(16, n).astype(F32)
        sb3[:, :, columns(p)] = total.astype(BF).reshape(4, 4, n)
        flights[p] = hop(p, 2)
    for p in range(3):
        off, n, order = PARTS[p]
        for copy in flights[p]:
            copy.wait_recv()
        total = sb3[coord[order[0]], :, columns(p)].astype(F32)
        for k in range(3):
            total += rb3[k, :, columns(p)].astype(F32)
        out[:, off : off + n] = (hidden[:, off : off + n] + total).astype(BF)
    for copy in sent:
        copy.wait_send()


def per_device(
    tokens, lengths, cache_keys, cache_values, query_w, key_w, value_w, out_w, mix_lambda, head_gain,
    attn_gain, ffn_gain, routes, route_weights, exp_gate, exp_up, exp_down,
    dense_gate, dense_up, dense_down, branch_gate,
):
    def vm(*shape, dtype=BF):
        return pltpu.VMEM(shape, dtype)

    dma = pltpu.SemaphoreType.DMA
    scratch = [
        vm(4, D), vm(1, 4, dtype=jnp.int32), vm(4, 2048, 128), vm(4, 2048, 128),
        vm(D, 1024), vm(D, 256), vm(D, 256), vm(1024, D),
        vm(1, 8, dtype=F32), vm(1, 128, dtype=F32), vm(1, D, dtype=F32), vm(1, D, dtype=F32),
        vm(2, 4, dtype=jnp.int32), vm(2, 4, dtype=F32), vm(16, 128),
        vm(3, D, 256), vm(512, D), vm(2, 128, D), vm(352, 256), vm(352, 256), vm(352, 256),
        vm(8, 3, PAD, 256), vm(8, 4, 128, dtype=F32), vm(4, 8, 128, dtype=F32),
        vm(2, 4, 4, 4, 4, D + META), vm(2, 256, D + META), vm(4, 512, 128),
        vm(4, 4, 4, 4, D), vm(4, 4, 4, 4, D), vm(256, D, dtype=F32), vm(4, 4, 4, 4, D),
        vm(3, 4, 4, 4, D), vm(4, 4, 4, D), vm(3, 4, 4, D), vm(4, 4, D), vm(3, 4, D),
        dma((21,)), dma((12,)), dma((7,)), dma((2,)),
        dma((2, 7)), dma((2, 7)), dma((3, 3, 3)), dma((3, 3, 3)), dma((3, 4)), dma((3, 4)),
        dma((3,)), dma((3,)), dma((3, 3, 3)), dma((3, 3, 3)),
    ]
    return pl.pallas_call(
        kernel,
        out_shape=(vm(4, D), vm(4, 256), vm(4, 256)),
        in_specs=[pl.BlockSpec(memory_space=pl.ANY)] * 21,
        out_specs=[pl.BlockSpec(memory_space=pltpu.VMEM)] * 3,
        scratch_shapes=scratch,
        compiler_params=pltpu.CompilerParams(
            collective_id=0, has_side_effects=True, vmem_limit_bytes=56 * 1024 * 1024
        ),
        name="layer",
    )(
        tokens, lengths.reshape(1, 4), cache_keys.reshape(4, 2048, 128), cache_values.reshape(4, 2048, 128),
        query_w, key_w, value_w, out_w, mix_lambda.reshape(1, 8), head_gain.reshape(1, 128),
        attn_gain.reshape(1, D), ffn_gain.reshape(1, D), routes.T, route_weights.T,
        exp_gate, exp_up, exp_down, dense_gate.transpose(0, 2, 1), dense_up.transpose(0, 2, 1), dense_down, branch_gate.reshape(16, 128),
    )


def solution(mesh):
    placed = (
        P("ep", None), P("ep"), P("ep", None, None, None), P("ep", None, None, None),
        P(), P(), P(), P(), P(), P(), P(), P(),
        P("ep", None), P("ep", None), P(None, "ep"), P(None, "ep"), P("ep", None),
        P("ep", None, None), P("ep", None, None), P("ep", None, None), P(),
    )
    return jax.shard_map(
        per_device,
        mesh=mesh,
        in_specs=placed,
        out_specs=(P("ep", None), P("ep", None), P("ep", None)),
        check_vma=False,
    )
```

```python
import jax
import jax.numpy as jnp
from jax import lax
from jax.experimental import pallas as pl
from jax.experimental.pallas import tpu as pltpu
from jax.sharding import PartitionSpec as P

BF = jnp.bfloat16
F32 = jnp.float32
MESH = pl.DeviceIdType.MESH
ALL = slice(None)
D = 2048
META = 128
HID = 384
PAD = 48
PARTS = ((0, 768, "xyz"), (768, 640, "yzx"), (1408, 640, "zxy"))
STRIDE = {"x": 2, "y": 8, "z": 32}
NT = (((1,), (1,)), ((), ()))


def pick(**at):
    return tuple(at.get(axis, ALL) for axis in "zyx")


def to_col(row):
    n = row.shape[1]
    same = lax.broadcasted_iota(jnp.int32, (n, n), 0) == lax.broadcasted_iota(jnp.int32, (n, n), 1)
    return jnp.sum(jnp.where(same, jnp.broadcast_to(row, (n, n)), 0.0), axis=1, keepdims=True)


def kernel(
    tokens, lengths, keys, values, query_w, key_w, value_w, out_w, mix_lambda, head_gain,
    attn_gain, ffn_gain, routes, route_weights, exp_gate, exp_up, exp_down,
    dense_gate, dense_up, dense_down, branch_gate,
    out, new_keys, new_values,
    tok_v, len_v, k_v, v_v, wq_v, wk_v, wv_v, wo_v, lam_v, hg_v, ag_v, fg_v, rt_v, rw_v, bg_v,
    w1, w2, dgu, qs, hs, xa, xf, act, pd, rs0, sb1, rb1, sb2, rb2,
    load_sem, qkv_sem, w_sem, ds_sem, dd_sem, ag_send, ag_recv, dx_recv, rd_recv, rs_send, rs1_recv, rs2_recv,
):
    me = lax.axis_index("ep")
    core = lax.rem(me, 2)
    coord = {
        "x": lax.rem(lax.div(me, 2), 4),
        "y": lax.rem(lax.div(me, 8), 4),
        "z": lax.div(me, 32),
    }
    block = lax.div(me, 16)
    column = lax.rem(me, 16)
    partner = me + 1 - 2 * core

    def along(axis, k):
        there = lax.rem(coord[axis] + k, 4)
        return me + (there - coord[axis]) * STRIDE[axis], there

    def across(one, k, two, l):
        first, second = lax.rem(coord[one] + k, 4), lax.rem(coord[two] + l, 4)
        to = me + (first - coord[one]) * STRIDE[one] + (second - coord[two]) * STRIDE[two]
        return to, first, second

    barrier = pltpu.get_barrier_semaphore()
    friends = [partner]
    for axis in "xyz":
        for k in (1, 2, 3):
            friends.append(along(axis, k)[0])
    for one, two in ("xy", "yz", "zx"):
        for k in (1, 2, 3):
            for l in (1, 2, 3):
                friends.append(across(one, k, two, l)[0])
    for friend in friends:
        pl.semaphore_signal(barrier, inc=1, device_id=(friend,), device_id_type=MESH)

    def remote(src, dst, send, recv, to):
        return pltpu.make_async_remote_copy(
            src_ref=src, dst_ref=dst, send_sem=send, recv_sem=recv, device_id=(to,), device_id_type=MESH
        )

    def load(src, dst, sem):
        copy = pltpu.make_async_copy(src, dst, sem)
        copy.start()
        return copy

    def load_all(pairs, sem):
        return [load(src, dst, sem) for src, dst in pairs]

    def finish(copies):
        for copy in copies:
            copy.wait()

    first = [load(tokens, tok_v, load_sem.at[0]), load(attn_gain, ag_v, load_sem.at[1])]
    step = D // 4
    qkv_loads = []
    for i in range(4):
        rows = pl.ds(i * step, step)
        qkv_loads.append(
            [
                load(query_w.at[rows], wq_v.at[rows], qkv_sem.at[i, 0]),
                load(key_w.at[rows], wk_v.at[rows], qkv_sem.at[i, 1]),
                load(value_w.at[rows], wv_v.at[rows], qkv_sem.at[i, 2]),
            ]
        )
    small = [
        load(src, dst, load_sem.at[5 + i])
        for i, (src, dst) in enumerate(
            (
                (lengths, len_v), (mix_lambda, lam_v), (head_gain, hg_v),
                (ffn_gain, fg_v), (routes, rt_v), (route_weights, rw_v), (branch_gate, bg_v),
            )
        )
    ]
    k_load = load(keys, k_v, load_sem.at[12])
    dgu[:, PAD:, :] = jnp.zeros((2, 128 - PAD, D), BF)
    w2[HID + PAD :, :] = jnp.zeros((128 - PAD, D), BF)

    own_cols = pl.ds(pl.multiple_of(block * 256, 256), 256)

    def units(there):
        return pl.ds(pl.multiple_of(lax.div(there, 2) * 88 + lax.rem(there, 2) * 40, 8), PAD)

    def hand_out(pairs, sems):
        for k in range(1, 8):
            there = lax.rem(block + k, 8)
            for src, dst in pairs:
                remote(src.at[0, units(there)], dst, sems.at[0], sems.at[1], there * 16 + column).start()

    up_pairs = (
        (dense_gate, dgu.at[0, pl.ds(0, PAD), own_cols]),
        (dense_up, dgu.at[1, pl.ds(0, PAD), own_cols]),
    )
    down_pairs = ((dense_down, w2.at[pl.ds(HID, PAD), own_cols]),)
    own_loads = [
        load(src.at[0, units(block)], dst, load_sem.at[2 + i])
        for i, (src, dst) in enumerate(up_pairs + down_pairs)
    ]
    finish(first)
    x = tok_v[...].astype(F32)
    normed = (x * lax.rsqrt(jnp.mean(x * x, axis=1, keepdims=True) + 1e-6) * ag_v[...]).astype(BF)

    query = jnp.zeros((4, 1024), F32)
    key = jnp.zeros((4, 256), F32)
    value = jnp.zeros((4, 256), F32)
    for i in range(4):
        finish(qkv_loads[i])
        if i == 0:
            v_load = load(values, v_v, load_sem.at[13])
        if i == 2:
            o_load = load(out_w, wo_v, load_sem.at[14])
            pl.semaphore_wait(barrier, len(friends))
            hand_out(up_pairs, ds_sem)
        part = normed[:, i * step : (i + 1) * step]
        rows = pl.ds(i * step, step)
        query += jnp.dot(part, wq_v[rows, :], preferred_element_type=F32)
        key += jnp.dot(part, wk_v[rows, :], preferred_element_type=F32)
        value += jnp.dot(part, wv_v[rows, :], preferred_element_type=F32)
    key = key.astype(BF)
    value = value.astype(BF)
    new_keys[...] = key
    new_values[...] = value
    key = key.astype(F32)
    value = value.astype(F32)
    query = query.astype(BF).astype(F32)
    for h in range(8):
        qs[h] = query[:, h * 128 : (h + 1) * 128]

    w_loads = []
    for n in range(3):
        cols = pl.ds(n * 128, 128)
        w_loads.append(load(exp_gate.at[:, cols], w1.at[n, :, pl.ds(0, 128)], w_sem.at[2 * n]))
        w_loads.append(load(exp_up.at[:, cols], w1.at[n, :, pl.ds(128, 128)], w_sem.at[2 * n + 1]))
    w_loads.append(load(exp_down, w2.at[pl.ds(0, HID)], w_sem.at[6]))
    finish(small)
    k_load.wait()
    lam = to_col(lam_v[...])
    row8 = lax.broadcasted_iota(jnp.int32, (8, 128), 0)
    lane8 = lax.broadcasted_iota(jnp.int32, (8, 128), 1)
    row16 = lax.rem(lax.broadcasted_iota(jnp.int32, (16, 2048), 0), 8)
    spot = lax.broadcasted_iota(jnp.int32, (16, 2048), 1)
    place = jnp.where(lax.rem(spot, 2) == lax.div(row16, 4), spot, 2 * D)
    scores = []
    owns = []
    for s in range(4):
        heads_q = qs[:, s, :]
        q16 = jnp.concatenate(
            [jnp.where(lane8 < 64, heads_q, 0.0), jnp.where(lane8 >= 64, heads_q, 0.0)], axis=0
        )
        own_key = jnp.where(row8 < 4, key[s : s + 1, :128], key[s : s + 1, 128:])
        score = lax.dot_general(q16.astype(BF), k_v[s], NT, preferred_element_type=F32) * 0.125
        scores.append(jnp.where(place < 2 * len_v[0:1, s : s + 1], score, -jnp.inf))
        owns.append(
            jnp.sum(q16 * jnp.concatenate([own_key, own_key], axis=0), axis=1, keepdims=True) * 0.125
        )
    weights = []
    own_weights = []
    for s in range(4):
        largest = jnp.maximum(jnp.max(scores[s], axis=1, keepdims=True), owns[s])
        raised = jnp.exp(scores[s] - largest)
        own_raised = jnp.exp(owns[s] - largest)
        share = 1.0 / (jnp.sum(raised, axis=1, keepdims=True) + own_raised)
        first_share, second_share = share[:8], lam * share[8:]
        weights.append((raised[:8] * first_share - raised[8:] * second_share).astype(BF))
        own_weights.append(
            (own_raised[:8] * first_share - own_raised[8:] * second_share).astype(BF).astype(F32)
        )
    v_load.wait()
    for s in range(4):
        own_value = jnp.where(row8 < 4, value[s : s + 1, :128], value[s : s + 1, 128:])
        mixed = jnp.dot(weights[s], v_v[s], preferred_element_type=F32) + own_weights[s] * own_value
        hs[s] = mixed * lax.rsqrt(jnp.mean(mixed * mixed, axis=1, keepdims=True) + 1e-5) * hg_v[...]
    heads = jnp.concatenate([hs[:, h, :] for h in range(8)], axis=1).astype(BF)
    o_load.wait()
    hidden = x + jnp.dot(heads, wo_v[...], preferred_element_type=F32)
    ffn_in = (
        hidden * lax.rsqrt(jnp.mean(hidden * hidden, axis=1, keepdims=True) + 1e-6) * fg_v[...]
    ).astype(BF)
    gate_w = bg_v[...].astype(F32)
    toward = jnp.zeros((4, 128), F32)
    for j in range(16):
        toward += ffn_in[:, j * 128 : (j + 1) * 128].astype(F32) * gate_w[j : j + 1]
    gate = jax.nn.sigmoid(jnp.sum(toward, axis=1, keepdims=True))
    lane4 = lax.broadcasted_iota(jnp.int32, (4, META), 1)
    expert4 = lax.rem(lane4, 8)
    scale = jnp.where(lane4 < 16, 0.0, gate)
    for j in range(2):
        named = to_col(rt_v[j : j + 1, :].astype(F32)).astype(jnp.int32)
        scale += jnp.where((expert4 == named) & (lane4 < 16), to_col(rw_v[j : j + 1, :]), 0.0)
    upper = scale.astype(BF).astype(F32)
    meta = jnp.where(
        (lane4 < 8) | (lane4 == 16), upper, jnp.where((lane4 < 16) | (lane4 == 17), scale - upper, 0.0)
    ).astype(BF)
    mine = (coord["z"], coord["y"], coord["x"])
    xa[(core,) + mine] = jnp.concatenate([ffn_in, meta], axis=1)

    def width(p):
        off, n, order = PARTS[p]
        return pl.ds(off, n + META if p == 2 else n)

    def piece(p, half, **at):
        return xa.at[(half,) + pick(**at) + (ALL, width(p))]

    def behind(axis, k):
        return lax.rem(coord[axis] + 4 - k, 4)

    for line in (2, 1, 3, 0):
        for k in (2, 1, 3, 0):
            for p in range(3):
                a1, a2, a3 = PARTS[p][2]
                if line or k:
                    ref = piece(p, core, **coord)
                    send = ag_send.at[1 if line else 0]
                    remote(ref, ref, send, ag_recv.at[p, 0, line], across(a1, k, a2, line)[0]).start()
    for line in (0, 1, 3, 2):
        for p in range(3):
            a1, a2, a3 = PARTS[p][2]
            ref = piece(p, core, **{a2: behind(a2, line), a3: coord[a3]})
            came = ref if line else piece(p, core, **{a1: pl.ds(0, 3), a2: coord[a2], a3: coord[a3]})
            remote(came, came, ag_send.at[1], ag_recv.at[p, 0, line], partner).wait_recv()
            for k in (2, 1, 3):
                remote(ref, ref, ag_send.at[2], ag_recv.at[p, 1, line], along(a3, k)[0]).start()
    hand_out(down_pairs, dd_sem)
    for line in (0, 1, 3, 2):
        for p in range(3):
            a1, a2, a3 = PARTS[p][2]
            three = piece(p, core, **{a2: behind(a2, line), a3: pl.ds(0, 3)})
            remote(three, three, ag_send.at[2], ag_recv.at[p, 1, line], partner).wait_recv()
            ref = piece(p, core, **{a2: behind(a2, line)})
            remote(ref, ref, ag_send.at[3], dx_recv.at[p, line], partner).start()

    def settle(half):
        def body(z, carry):
            rows = pl.ds(pl.multiple_of(z * 64, 64), 64)
            xf[half, rows, :] = xa[half, z].reshape(64, D + META)
            return carry

        lax.fori_loop(0, 4, body, 0)

    for copy in w_loads:
        copy.wait()
    finish(own_loads)
    came = dgu.at[:, pl.ds(0, PAD), pl.ds(0, 7 * 256)]
    remote(came, came, ds_sem.at[0], ds_sem.at[1], partner).wait_recv()
    lane = lax.broadcasted_iota(jnp.int32, (256, META), 1)
    spare = (lane >= 8 * lax.rem(block, 2)) & (lane < PAD)

    def hidden_units(half):
        settle(half)
        scales = xf[half, :, D:].astype(F32)
        route = jnp.sum(jnp.where((lane == block) | (lane == block + 8), scales, 0.0), axis=1, keepdims=True)
        dense = jnp.sum(jnp.where((lane == 16) | (lane == 17), scales, 0.0), axis=1, keepdims=True)
        for n in range(3):
            both = jnp.dot(xf[half, :, :D], w1[n], preferred_element_type=F32)
            g, u = both[:, :128], both[:, 128:]
            act[half, :, n * 128 : (n + 1) * 128] = (g * jax.nn.sigmoid(g) * u * route).astype(BF)
        both = lax.dot_general(xf[half, :, :D], dgu[...].reshape(256, D), NT, preferred_element_type=F32)
        g, u = both[:, :128], both[:, 128:]
        act[half, :, HID:] = jnp.where(spare, g * jax.nn.sigmoid(g) * u * dense, 0.0).astype(BF)

    def partner_rows():
        for line in (0, 1, 3, 2):
            for p in range(3):
                a1, a2, a3 = PARTS[p][2]
                ref = piece(p, 1 - core, **{a2: behind(a2, line)})
                remote(ref, ref, ag_send.at[3], dx_recv.at[p, line], partner).wait_recv()

    pl.when(core == 0)(partner_rows)
    hidden_units(1)
    pl.when(core == 1)(partner_rows)
    hidden_units(0)
    came = w2.at[pl.ds(HID, PAD), pl.ds(0, 7 * 256)]
    remote(came, came, dd_sem.at[0], dd_sem.at[1], partner).wait_recv()

    def columns(p, h=None):
        off, n, order = PARTS[p]
        return pl.ds(off, n) if h is None else pl.ds(off + 256 * h, 256 if h == 0 else n - 256)

    def product(half, cols):
        return jnp.dot(act[half], w2[:, cols], preferred_element_type=F32)

    def swap(p, h):
        cols = columns(p, h)
        return remote(pd.at[:, cols], rs0.at[:, cols], rs_send.at[0], rd_recv.at[p, h], partner)

    for h in range(2):
        for p in range(3):
            cols = columns(p, h)
            pd[:, cols] = product(1 - core, cols).astype(BF)
            swap(p, h).start()
    for h in range(2):
        for p in range(3):
            a1, a2, a3 = PARTS[p][2]
            cols = columns(p, h)
            near = product(core, cols)
            swap(p, h).wait_recv()
            far = rs0[:, cols].astype(F32)
            sb1[:, :, :, :, cols] = (near + far).astype(BF).reshape(4, 4, 4, 4, cols.size)
            for k in (2, 1, 3):
                to, there = along(a3, k)
                src = sb1.at[pick(**{a3: there}) + (ALL, cols)]
                remote(src, rb1.at[k - 1, :, :, :, cols], rs_send.at[1], rs1_recv.at[p, h], to).start()

    def in_plane(p, c1, c2):
        a1, a2, a3 = PARTS[p][2]
        return (c1, c2) if "zyx".index(a1) < "zyx".index(a2) else (c2, c1)

    for h in range(2):
        for p in range(3):
            a1, a2, a3 = PARTS[p][2]
            cols = columns(p, h)
            three = rb1.at[:, :, :, :, cols]
            remote(three, three, rs_send.at[1], rs1_recv.at[p, h], partner).wait_recv()
            total = sb1[pick(**{a3: coord[a3]}) + (ALL, cols)].reshape(64, cols.size).astype(F32)
            for k in range(3):
                total += rb1[k, :, :, :, cols].reshape(64, cols.size).astype(F32)
            sb2[:, :, :, cols] = total.astype(BF).reshape(4, 4, 4, cols.size)
            for k in (2, 1, 3, 0):
                for l in (2, 1, 3, 0):
                    if k or l:
                        to, c1, c2 = across(a1, k, a2, l)
                        src = sb2.at[in_plane(p, c1, c2) + (ALL, cols)]
                        remote(src, rb2.at[k * 4 + l - 1, :, cols], rs_send.at[2], rs2_recv.at[p], to).start()
    for p in range(3):
        off, n, (a1, a2, a3) = PARTS[p]
        cols = columns(p)
        most = rb2.at[:, :, cols]
        remote(most, most, rs_send.at[2], rs2_recv.at[p], partner).wait_recv()
        total = sb2[in_plane(p, coord[a1], coord[a2]) + (ALL, cols)].astype(F32)
        for k in range(15):
            total += rb2[k, :, cols].astype(F32)
        out[:, off : off + n] = (hidden[:, off : off + n] + total).astype(BF)
    for ref, sem in (
        (dgu.at[:, pl.ds(0, PAD), pl.ds(0, 7 * 256)], ds_sem.at[0]),
        (w2.at[pl.ds(HID, PAD), pl.ds(0, 7 * 256)], dd_sem.at[0]),
        (xa.at[0, 0, 0, pl.ds(0, 3)], ag_send.at[0]),
        (xa.at[0, 0, pl.ds(0, 3)], ag_send.at[1]),
        (xa.at[0, pl.ds(0, 3)], ag_send.at[2]),
        (xa.at[0], ag_send.at[3]),
        (pd, rs_send.at[0]),
        (sb1.at[pl.ds(0, 3)], rs_send.at[1]),
        (rb2, rs_send.at[2]),
    ):
        remote(ref, ref, sem, rs2_recv.at[0], partner).wait_send()


def per_device(
    tokens, lengths, cache_keys, cache_values, query_w, key_w, value_w, out_w, mix_lambda, head_gain,
    attn_gain, ffn_gain, routes, route_weights, exp_gate, exp_up, exp_down,
    dense_gate, dense_up, dense_down, branch_gate,
):
    def vm(*shape, dtype=BF):
        return pltpu.VMEM(shape, dtype)

    dma = pltpu.SemaphoreType.DMA
    scratch = [
        vm(4, D), vm(1, 4, dtype=jnp.int32), vm(4, 2048, 128), vm(4, 2048, 128),
        vm(D, 1024), vm(D, 256), vm(D, 256), vm(1024, D),
        vm(1, 8, dtype=F32), vm(1, 128, dtype=F32), vm(1, D, dtype=F32), vm(1, D, dtype=F32),
        vm(2, 4, dtype=jnp.int32), vm(2, 4, dtype=F32), vm(16, 128),
        vm(3, D, 256), vm(512, D), vm(2, 128, D), vm(8, 4, 128, dtype=F32), vm(4, 8, 128, dtype=F32),
        vm(2, 4, 4, 4, 4, D + META), vm(2, 256, D + META), vm(2, 256, HID + 128),
        vm(256, D), vm(256, D), vm(4, 4, 4, 4, D),
        vm(3, 4, 4, 4, D), vm(4, 4, 4, D), vm(15, 4, D),
        dma((17,)), dma((4, 3)), dma((7,)), dma((2,)), dma((2,)), dma((4,)), dma((3, 2, 4)), dma((3, 4)), dma((3, 2)),
        dma((3,)), dma((3, 2)), dma((3,)),
    ]
    return pl.pallas_call(
        kernel,
        out_shape=(vm(4, D), vm(4, 256), vm(4, 256)),
        in_specs=[pl.BlockSpec(memory_space=pl.ANY)] * 21,
        out_specs=[pl.BlockSpec(memory_space=pltpu.VMEM)] * 3,
        scratch_shapes=scratch,
        compiler_params=pltpu.CompilerParams(
            collective_id=0, has_side_effects=True, vmem_limit_bytes=56 * 1024 * 1024
        ),
        name="layer",
    )(
        tokens, lengths.reshape(1, 4), cache_keys.reshape(4, 2048, 128), cache_values.reshape(4, 2048, 128),
        query_w, key_w, value_w, out_w, mix_lambda.reshape(1, 8), head_gain.reshape(1, 128),
        attn_gain.reshape(1, D), ffn_gain.reshape(1, D), routes.T, route_weights.T,
        exp_gate, exp_up, exp_down, dense_gate.transpose(0, 2, 1), dense_up.transpose(0, 2, 1), dense_down, branch_gate.reshape(16, 128),
    )


def solution(mesh):
    placed = (
        P("ep", None), P("ep"), P("ep", None, None, None), P("ep", None, None, None),
        P(), P(), P(), P(), P(), P(), P(), P(),
        P("ep", None), P("ep", None), P(None, "ep"), P(None, "ep"), P("ep", None),
        P("ep", None, None), P("ep", None, None), P("ep", None, None), P(),
    )
    return jax.shard_map(
        per_device,
        mesh=mesh,
        in_specs=placed,
        out_specs=(P("ep", None), P("ep", None), P("ep", None)),
        check_vma=False,
    )
```
